32 devices in a mesh: fs: 4 (over y, x), tp: 8 (over z, core).
Axes of the slice: x: 2, y: 2, z: 4, core: 2. Of those that a mesh axis runs over, the one named last changes fastest.
Arguments:
- stream_in: bfloat16 [4096, 4096], P(('fs', 'tp')), may hold values from -6 to 6
- mixer_out: bfloat16 [4096, 4096], P(('fs', 'tp')), may hold values from -6 to 6
- mix_gain: float32 [4096], replicated, may hold values from 0.1 to 1.9
- pre_gain: float32 [4096], replicated, may hold values from 0.1 to 1.9
- gate_weight: float32 [4096, 6144], P('fs', 'tp'), may hold values from -0.09375 to 0.09375
- up_weight: float32 [4096, 6144], P('fs', 'tp'), may hold values from -0.09375 to 0.09375
- gate_scale: float32 [6144], P('tp'), may hold values from 0.5 to 2
- up_scale: float32 [6144], P('tp'), may hold values from 0.5 to 2
Outputs:
- hidden: bfloat16 [4096, 6144], P('fs', 'tp')
- stream: bfloat16 [4096, 4096], P(('fs', 'tp'))
The draws below stay inside these ranges and needn't reach their ends.
All inputs are finite; a program needn't handle non-finite values.
Results may differ from the reference program's by a relative error of at most 0.0082.
Values may be sent and summed in bfloat16 or wider, within the bound.
No kernel may reach another device: no remote copies, remote signals or barrier semaphores. Data moves between devices by JAX's collectives and lax.ppermute only.
A program may use at most 128 MiB of HBM per device.

```python
import math
import jax
import jax.numpy as jnp
from jax import lax

D = 4096
FF = 6144
TOKENS = 4096


def levels(rng, shape, split, low, largest):
    def one(dim, shards_of):
        steps = jax.random.uniform(jax.random.fold_in(jax.random.fold_in(rng, 6), dim), (shards_of,), jnp.float32, low / len(split), largest / len(split))
        return jnp.repeat(jnp.exp(steps), shape[dim] // shards_of).reshape((-1,) + (1,) * (len(shape) - dim - 1))

    level = one(*split[0])
    for cut in split[1:]:
        level = level * one(*cut)
    return level


def centred(key, extent, width, limit, pieces=(), kind=jnp.bfloat16):
    entries = jax.random.normal(key, extent, jnp.float32) * width
    if len(pieces) > 0:
        entries = levels(key, extent, pieces, -0.22, 0.18) * entries
    return jnp.clip(entries, min=-limit, max=limit).astype(kind)


def setup_inputs(seed: int = 0) -> dict:
    splits = jax.random.split(jax.random.key(seed), 9)
    stream_in = centred(splits[0], (TOKENS, D), 1.0, 6.0, ((0, 32),))
    mixer_out = centred(splits[1], (TOKENS, D), 1.0, 6.0, ((0, 32),))
    mix_gain = jnp.clip(1.0 + 0.18 * jax.random.normal(splits[2], (D,), jnp.float32), 0.1, 1.9)
    pre_gain = jnp.clip(1.0 + 0.18 * jax.random.normal(splits[3], (D,), jnp.float32), 0.1, 1.9)
    gate_weight = centred(splits[4], (D, FF), D ** -0.5, 0.09375, ((0, 4), (1, 8)), jnp.float32)
    up_weight = centred(splits[5], (D, FF), D ** -0.5, 0.09375, ((0, 4), (1, 8)), jnp.float32)
    gate_scale = jnp.clip(jnp.exp(math.log(2.0) - 1.3862944 * jax.random.uniform(splits[6], (FF,), jnp.float32) ** levels(splits[6], (FF,), ((0, 8),), -0.2, 0.2)), 0.5, 2.0)
    up_scale = jnp.clip(jnp.exp(math.log(2.0) - 1.3862944 * jax.random.uniform(splits[7], (FF,), jnp.float32) ** levels(splits[7], (FF,), ((0, 8),), -0.2, 0.2)), 0.5, 2.0)
    return {"stream_in": stream_in, "mixer_out": mixer_out, "mix_gain": mix_gain, "pre_gain": pre_gain, "gate_weight": gate_weight, "up_weight": up_weight, "gate_scale": gate_scale, "up_scale": up_scale}


epsilon = 1e-06

def rms_scaled(values, gain):
    return values * lax.rsqrt(lax.optimization_barrier(jnp.mean(values * values, axis=-1, keepdims=True)) + epsilon) * gain

def reference(stream_in, mixer_out, mix_gain, pre_gain, gate_weight, up_weight, gate_scale, up_scale):
    mixed = stream_in.astype(jnp.float32) + rms_scaled(mixer_out.astype(jnp.float32), mix_gain)
    stream = mixed.astype(jnp.bfloat16)
    normed = rms_scaled(stream.astype(jnp.float32), pre_gain).astype(jnp.bfloat16)
    gate = jnp.dot(normed, gate_weight.astype(jnp.bfloat16), preferred_element_type=jnp.float32) * gate_scale
    up = jnp.dot(normed, up_weight.astype(jnp.bfloat16), preferred_element_type=jnp.float32) * up_scale
    hidden = (jax.nn.silu(gate) * up).astype(jnp.bfloat16)
    return (hidden, stream)
```

```python
import math

import jax
import jax.numpy as jnp
from jax import lax
from jax.experimental import pallas as pl
from jax.experimental.pallas import tpu as pltpu
from jax.sharding import PartitionSpec as P


epsilon = 1e-06
CHUNK = 128
ANY = pl.BlockSpec(memory_space=pltpu.HBM)


def rms_scaled(values, gain):
    return values * lax.rsqrt(jnp.mean(values * values, axis=-1, keepdims=True) + epsilon) * gain


def cast(gate_weight, up_weight, j, c):
    k = gate_weight.shape[0]

    def body(g, u, top, bottom):
        for half, out in enumerate((top, bottom)):
            rows = slice(half * (k // 2), (half + 1) * (k // 2))
            out[:, :c] = g[rows].astype(out.dtype)
            out[:, c:] = u[rows].astype(out.dtype)

    spec = pl.BlockSpec((k, c), lambda i: (0, j))
    whole = pl.BlockSpec((k // 2, 2 * c), lambda i: (0, 0))
    shape = jax.ShapeDtypeStruct((k // 2, 2 * c), jnp.bfloat16)
    return pl.pallas_call(
        body, grid=(1,), in_specs=[spec, spec], out_specs=[whole, whole], out_shape=[shape, shape]
    )(gate_weight, up_weight)


def pack(gate_scale, up_scale):
    def body(g, u, out):
        out[0:1] = g[...]
        out[1:2] = u[...]

    return pl.pallas_call(
        body,
        out_shape=jax.ShapeDtypeStruct((2, gate_scale.shape[1]), jnp.float32),
        name="pack",
    )(gate_scale, up_scale)


def assemble(slots, mates, chips):
    rows, width = slots[0].shape
    n = 2 * chips - 1

    def body(*refs):
        out, sem = refs[2 * n], refs[2 * n + 1]
        t = lax.axis_index("tp")
        z, core = t // 2, t % 2

        def copies(fn):
            for side in range(2):
                for i in range(n):
                    source = z + i - (chips - 1)

                    @pl.when((source >= 0) & (source < chips))
                    def _():
                        lane = core if side == 0 else 1 - core
                        at = pl.multiple_of((2 * source + lane) * rows, rows)
                        fn(
                            pltpu.make_async_copy(
                                refs[side * n + i], out.at[pl.ds(at, rows)], sem.at[side, i]
                            )
                        )

        copies(lambda c: c.start())
        copies(lambda c: c.wait())

    return pl.pallas_call(
        body,
        in_specs=[ANY] * (2 * n),
        out_specs=ANY,
        out_shape=jax.ShapeDtypeStruct((2 * chips * rows, width), slots[0].dtype),
        scratch_shapes=[pltpu.SemaphoreType.DMA((2, n))],
        name="assemble",
    )(*slots, *mates)


def project(tokens, pieces, scales, hidden, index, fa, fb, width):
    m, k = tokens.shape
    half, two_c = pieces[0][3].shape
    c = two_c // 2
    tm = min(256, m)
    n = len(pieces)

    def body(a, scale, *rest):
        parts, rest = rest[:n], rest[n:]
        if hidden is not None:
            rest = rest[1:]
        out, w, sem = rest

        @pl.when(pl.program_id(0) == 0)
        def _():
            f = lax.axis_index("fs")
            y, x = f // fa, f % fa

            def copy(i):
                h, dx, dy, _ = pieces[i]
                owner = ((y + fb - dy) % fb) * fa + (x + fa - dx) % fa
                at = pl.multiple_of((2 * owner + h) * half, half)
                return pltpu.make_async_copy(parts[i], w.at[pl.ds(at, half)], sem.at[i])

            for i in range(n):
                copy(i).start()
            for i in range(n):
                copy(i).wait()

        both = jnp.dot(a[...], w[...], preferred_element_type=jnp.float32)
        gate = both[:, :c] * scale[0:1]
        up = both[:, c:] * scale[1:2]
        out[...] = (gate / (1.0 + jnp.exp(-gate)) * up).astype(out.dtype)

    in_specs = [
        pl.BlockSpec((tm, k), lambda i: (i, 0)),
        pl.BlockSpec((2, c), lambda i: (0, index)),
    ] + [ANY] * n
    args = [tokens, scales] + [p[3] for p in pieces]
    aliases = {}
    if hidden is not None:
        aliases = {len(args): 0}
        in_specs.append(ANY)
        args.append(hidden)
    return pl.pallas_call(
        body,
        grid=(m // tm,),
        in_specs=in_specs,
        out_specs=pl.BlockSpec((tm, c), lambda i: (i, index)),
        out_shape=jax.ShapeDtypeStruct((m, width), jnp.bfloat16),
        scratch_shapes=[pltpu.VMEM((k, two_c), jnp.bfloat16), pltpu.SemaphoreType.DMA((n,))],
        input_output_aliases=aliases,
        cost_estimate=pl.CostEstimate(
            flops=2 * m * k * two_c,
            bytes_accessed=2 * (m * k + k * two_c + m * c),
            transcendentals=m * c,
        ),
    )(*args)


def solution(mesh):
    fs, tp = mesh.shape["fs"], mesh.shape["tp"]
    fa = math.isqrt(fs)
    fb = fs // fa
    chips = tp // 2
    along_x = [(y * fa + x, y * fa + (x + 1) % fa) for y in range(fb) for x in range(fa)]
    along_y = [(y * fa + x, ((y + 1) % fb) * fa + x) for y in range(fb) for x in range(fa)]
    swap = [(t, t ^ 1) for t in range(tp)]

    def ring(values, pairs, count):
        found = [values]
        for _ in range(count - 1):
            values = [lax.ppermute(v, "fs", pairs) for v in values]
            found.append(values)
        return found

    def gather(top, bottom):
        pieces = []
        first = [step[0] for step in ring([top], along_x, fa)]
        here = ring(first[:1], along_y, fb)
        there = ring(first[1:], along_y, fb)
        for dy in range(fb):
            pieces += [(0, dx, dy, v) for dx, v in enumerate(here[dy] + there[dy])]
        first = [step[0] for step in ring([bottom], along_y, fb)]
        here = ring(first[:1], along_x, fa)
        there = ring(first[1:], along_x, fa)
        for dx in range(fa):
            pieces += [(1, dx, dy, v) for dy, v in enumerate(here[dx] + there[dx])]
        return pieces

    def line(value):
        below, above = [], []
        low = high = value
        for s in range(1, chips):
            up = [(2 * z + c, 2 * z + 2 + c) for z in range(s - 1, chips - 1) for c in range(2)]
            down = [(2 * z + c, 2 * z - 2 + c) for z in range(1, chips - s + 1) for c in range(2)]
            low = lax.ppermute(low, "tp", up)
            high = lax.ppermute(high, "tp", down)
            below.append(low)
            above.append(high)
        return below[::-1] + [value] + above

    def on_device(
        stream_in, mixer_out, mix_gain, pre_gain, gate_weight, up_weight, gate_scale, up_scale
    ):
        mixed = stream_in.astype(jnp.float32) + rms_scaled(mixer_out.astype(jnp.float32), mix_gain)
        stream = mixed.astype(jnp.bfloat16)
        normed = rms_scaled(stream.astype(jnp.float32), pre_gain).astype(jnp.bfloat16)
        slots = line(normed)
        mates = []
        for v in slots:
            mates.append(lax.ppermute(v, "tp", swap))
        width = gate_weight.shape[1]
        gathered = []
        for j in range(width // CHUNK):
            top, bottom = cast(gate_weight, up_weight, j, CHUNK)
            gathered.append(gather(top, bottom))
        scales = pack(gate_scale[None], up_scale[None])
        tokens = assemble(slots, mates, chips)
        hidden = None
        for j, pieces in enumerate(gathered):
            hidden = project(tokens, pieces, scales, hidden, j, fa, fb, width)
        return (hidden, stream)

    return jax.shard_map(
        on_device,
        mesh=mesh,
        in_specs=(
            P(("fs", "tp"), None),
            P(("fs", "tp"), None),
            P(),
            P(),
            P("fs", "tp"),
            P("fs", "tp"),
            P("tp"),
            P("tp"),
        ),
        out_specs=(P("fs", "tp"), P(("fs", "tp"), None)),
        check_vma=False,
    )
```

```python
import math

import jax
import jax.numpy as jnp
from jax import lax
from jax.experimental import pallas as pl
from jax.experimental.pallas import tpu as pltpu
from jax.sharding import PartitionSpec as P


epsilon = 1e-06
LANES = 128
MIB = 1 << 20
ANY = pl.BlockSpec(memory_space=pl.ANY)


def grant(mib):
    return pltpu.CompilerParams(vmem_limit_bytes=mib * MIB)


def chunks(width):
    cuts = {0, min(LANES, width), max(width - 2 * LANES, 0), max(width - LANES, 0), width}
    cuts = sorted(cuts)
    return [(low, high - low) for low, high in zip(cuts, cuts[1:])]


def rms_scaled(values, gain):
    return values * lax.rsqrt(jnp.mean(values * values, axis=-1, keepdims=True) + epsilon) * gain


def norms(stream_in, mixer_out, mix_gain, pre_gain):
    m, d = stream_in.shape
    tm = min(32, m)

    def body(s, x, g, p, stream, normed):
        mixed = s[...].astype(jnp.float32) + rms_scaled(x[...].astype(jnp.float32), g[...])
        rounded = mixed.astype(jnp.bfloat16)
        stream[...] = rounded
        normed[...] = rms_scaled(rounded.astype(jnp.float32), p[...]).astype(jnp.bfloat16)

    rows = pl.BlockSpec((tm, d), lambda i: (i, 0))
    gain = pl.BlockSpec((1, d), lambda i: (0, 0))
    shape = jax.ShapeDtypeStruct((m, d), jnp.bfloat16)
    return pl.pallas_call(
        body,
        grid=(m // tm,),
        in_specs=[rows, rows, gain, gain],
        out_specs=[rows, rows],
        out_shape=[shape, shape],
        compiler_params=grant(8),
        name="norms",
    )(stream_in, mixer_out, mix_gain[None], pre_gain[None])


def cast(gate_weight, up_weight, parts, slabs, mib):
    k = gate_weight.shape[0]
    rows = k // slabs
    low, high = parts[0][0], parts[-1][0] + parts[-1][1]

    def body(g, u, *rest):
        outs, (held, sem) = rest[: len(parts)], rest[len(parts) :]

        def copy(i, side):
            cut = pl.ds(i * rows, rows)
            source = (g, u)[side].at[cut, pl.ds(low, high - low)]
            return pltpu.make_async_copy(source, held.at[side, cut], sem.at[side, i])

        for i in range(slabs):
            for side in range(2):
                copy(i, side).start()
        for i in range(slabs):
            cut = slice(i * rows, (i + 1) * rows)
            for side in range(2):
                copy(i, side).wait()
                for (at, c), out in zip(parts, outs):
                    part = held[side, cut, at - low : at - low + c]
                    out[cut, side * c : (side + 1) * c] = part.astype(out.dtype)

    return pl.pallas_call(
        body,
        in_specs=[ANY, ANY],
        out_specs=[pl.BlockSpec(memory_space=pltpu.VMEM)] * len(parts),
        out_shape=[pltpu.VMEM((k, 2 * c), jnp.bfloat16) for _, c in parts],
        scratch_shapes=[
            pltpu.VMEM((2, k, high - low), jnp.float32),
            pltpu.SemaphoreType.DMA((2, slabs)),
        ],
        compiler_params=grant(mib),
    )(gate_weight, up_weight)


def pack(gate_scale, up_scale):
    def body(g, u, out):
        out[0:1] = g[...]
        out[1:2] = u[...]

    return pl.pallas_call(
        body,
        out_shape=jax.ShapeDtypeStruct((2, gate_scale.shape[1]), jnp.float32),
        compiler_params=grant(1),
        name="pack",
    )(gate_scale, up_scale)


def by_distance(z, chips):
    return sorted(range(chips), key=lambda source: (abs(source - z), source))


def load(slots, mates, chips, ranks, fa, fb):
    rows, width = slots[0].shape
    local = width // (fa * fb)
    used = sorted(
        {by_distance(p, chips)[r] - p + chips - 1 for p in range(chips) for r in ranks}
    )
    n = len(used)

    def body(*refs):
        out, sem = refs[2 * n], refs[2 * n + 1]
        t, f = lax.axis_index("tp"), lax.axis_index("fs")
        z, core = t // 2, t % 2
        y, x = f // fa, f % fa

        def each(b, source, fn):
            da, db = b % fa, b // fa
            if fa == fb:
                da, db = jnp.where(core == 0, da, db), jnp.where(core == 0, db, da)
            owner = ((y + fb - db) % fb) * fa + (x + fa - da) % fa
            there = pl.ds(pl.multiple_of(owner * local, local), local)
            here = pl.ds(pl.multiple_of(b * local, local), local)
            for r in ranks:
                i = source[r]
                for side in range(2):
                    lane = core if side == 0 else 1 - core
                    at = pl.multiple_of((2 * (r - ranks[0]) + lane) * rows, rows)
                    fn(
                        pltpu.make_async_copy(
                            refs[side * n + i].at[:, there],
                            out.at[pl.ds(at, rows), here],
                            sem.at[side, r - ranks[0], b],
                        )
                    )

        for place in range(chips):

            @pl.when(z == place)
            def _():
                order = by_distance(place, chips)
                source = {r: used.index(order[r] - place + chips - 1) for r in ranks}
                for fn in (lambda c: c.start(), lambda c: c.wait()):

                    def step(b, carry):
                        each(b, source, fn)
                        return carry

                    lax.fori_loop(0, fa * fb, step, 0)

    return pl.pallas_call(
        body,
        in_specs=[ANY] * (2 * n),
        out_specs=pl.BlockSpec(memory_space=pltpu.VMEM),
        out_shape=pltpu.VMEM((2 * len(ranks) * rows, width), slots[0].dtype),
        scratch_shapes=[pltpu.SemaphoreType.DMA((2, len(ranks), fa * fb))],
        compiler_params=grant(1),
    )(*[slots[i] for i in used], *[mates[i] for i in used])


def near(tokens, groups):
    m = tokens.shape[0]
    local = groups[0][0].shape[0]
    n, count = len(groups[0]), len(groups)

    def body(a, *rest):
        parts, outs = rest[: n * count], rest[n * count :]
        for j, out in enumerate(outs):
            total = 0
            for b, part in enumerate(parts[j * n : (j + 1) * n]):
                cut = slice(b * local, (b + 1) * local)
                total += jnp.dot(a[:, cut], part[...], preferred_element_type=jnp.float32)
            out[...] = total

    vmem = pl.BlockSpec(memory_space=pltpu.VMEM)
    widths = [pieces[0].shape[1] for pieces in groups]
    return pl.pallas_call(
        body,
        in_specs=[vmem] * (n * count + 1),
        out_specs=[vmem] * count,
        out_shape=[pltpu.VMEM((m, w), jnp.float32) for w in widths],
        compiler_params=grant(14),
        cost_estimate=pl.CostEstimate(
            flops=2 * m * n * local * sum(widths), bytes_accessed=0, transcendentals=0
        ),
    )(tokens, *[piece for pieces in groups for piece in pieces])


def extend(tokens, totals, pieces):
    n = len(pieces)

    def body(*refs):
        rows, sums, parts, outs = refs[:2], refs[2:4], refs[4 : 4 + n], refs[4 + n :]
        for a, acc, out in zip(rows, sums, outs):
            both = acc[...]
            for (row, piece), part in zip(pieces, parts):
                cut = slice(row, row + piece.shape[0])
                both += jnp.dot(a[:, cut], part[...], preferred_element_type=jnp.float32)
            out[...] = both

    vmem = pl.BlockSpec(memory_space=pltpu.VMEM)
    return pl.pallas_call(
        body,
        in_specs=[vmem] * (4 + n),
        out_specs=[vmem] * 2,
        out_shape=[pltpu.VMEM(total.shape, jnp.float32) for total in totals],
        compiler_params=grant(8),
        cost_estimate=pl.CostEstimate(
            flops=sum(2 * t.size * p.shape[0] for t in totals for _, p in pieces),
            bytes_accessed=0,
            transcendentals=0,
        ),
    )(*tokens, *totals, *[piece for _, piece in pieces])


def final(tokens, totals, pieces, scales, hidden, at, c, chips, width):
    last = tokens[1].shape[0]
    m = tokens[0].shape[0] + last
    n = len(pieces)

    def body(*refs):
        rows, sums, scale, parts = refs[:2], refs[2:4], refs[4], refs[5 : 5 + n]
        out, block, sent = refs[-3:]
        z = lax.axis_index("tp") // 2

        def send(r, fn):
            for place in range(chips):

                @pl.when(z == place)
                def _():
                    q = by_distance(place, chips)[r]
                    fn(
                        pltpu.make_async_copy(
                            block.at[pl.ds(r * last, last)],
                            out.at[pl.ds(q * last, last), pl.ds(at, c)],
                            sent.at[r],
                        )
                    )

        for r in range(chips):
            side = int(r == chips - 1)
            low = 0 if side else r * last
            here = slice(low, low + last)
            both = sums[side][here]
            for (row, piece), part in zip(pieces, parts):
                cut = slice(row, row + piece.shape[0])
                both += jnp.dot(
                    rows[side][here, cut], part[...], preferred_element_type=jnp.float32
                )
            gate = both[:, :c] * scale[0:1, at : at + c]
            up = both[:, c:] * scale[1:2, at : at + c]
            held = (gate / (1.0 + jnp.exp(-gate)) * up).astype(block.dtype)
            block[r * last : (r + 1) * last] = held
            send(r, lambda d: d.start())
        for r in range(chips):
            send(r, lambda d: d.wait())

    vmem = pl.BlockSpec(memory_space=pltpu.VMEM)
    scratch = [pltpu.VMEM((m, c), jnp.bfloat16), pltpu.SemaphoreType.DMA((chips,))]
    args = [*tokens, *totals, scales] + [piece for _, piece in pieces]
    in_specs = [vmem] * len(args)
    aliases = {}
    if hidden is not None:
        aliases = {len(args): 0}
        in_specs.append(ANY)
        args.append(hidden)
    return pl.pallas_call(
        body,
        in_specs=in_specs,
        out_specs=ANY,
        out_shape=jax.ShapeDtypeStruct((m, width), jnp.bfloat16),
        scratch_shapes=scratch,
        input_output_aliases=aliases,
        compiler_params=grant(12),
        cost_estimate=pl.CostEstimate(
            flops=4 * c * m * sum(piece.shape[0] for _, piece in pieces),
            bytes_accessed=2 * m * c,
            transcendentals=m * c,
        ),
    )(*args)


def solution(mesh):
    fs, tp = mesh.shape["fs"], mesh.shape["tp"]
    fa = math.isqrt(fs)
    fb = fs // fa
    chips = tp // 2

    def along(axis):
        pairs = []
        for y in range(fb):
            for x in range(fa):
                for t in range(tp):
                    turn = axis ^ (t % 2) if fa == fb else axis
                    to = ((y + 1) % fb) * fa + x if turn else y * fa + (x + 1) % fa
                    pairs.append(((y * fa + x) * tp + t, to * tp + t))
        return pairs

    along_x, along_y = along(0), along(1)
    swap = [(t, t ^ 1) for t in range(tp)]

    def ring(value, pairs, count):
        found = []
        for _ in range(count - 1):
            value = lax.ppermute(value, ("fs", "tp"), pairs)
            found.append(value)
        return found

    def gather(value):
        half = value.shape[0] // 2
        xs = ring(value, along_x, fa)
        ys = ring(value, along_y, fb)
        pieces = [(0, 0, 0, value)]
        pieces += [(0, dx + 1, 0, v) for dx, v in enumerate(xs)]
        pieces += [(0, 0, dy + 1, v) for dy, v in enumerate(ys)]
        for dx, v in enumerate(xs):
            found = ring(v[:half], along_y, fb)
            pieces += [(0, dx + 1, dy + 1, u) for dy, u in enumerate(found)]
        for dy, v in enumerate(ys):
            found = ring(v[half:], along_x, fa)
            pieces += [(half, dx + 1, dy + 1, u) for dx, u in enumerate(found)]
        return pieces

    def line(value):
        below, above = [], []
        low = high = value
        for s in range(1, chips):
            up = [(2 * z + c, 2 * z + 2 + c) for z in range(s - 1, chips - 1) for c in range(2)]
            down = [(2 * z + c, 2 * z - 2 + c) for z in range(1, chips - s + 1) for c in range(2)]
            low = lax.ppermute(low, "tp", up)
            high = lax.ppermute(high, "tp", down)
            below.append(low)
            above.append(high)
        return below[::-1] + [value] + above

    def on_device(
        stream_in, mixer_out, mix_gain, pre_gain, gate_weight, up_weight, gate_scale, up_scale
    ):
        width = gate_weight.shape[1]
        stream, normed = norms(stream_in, mixer_out, mix_gain, pre_gain)
        slots = line(normed)
        mates = []
        for v in slots:
            mates.append(lax.ppermute(v, "tp", swap))
        parts = chunks(width)
        mine = []
        for i, some in enumerate((parts[:1], parts[1:])):
            if some:
                mine += cast(gate_weight, up_weight, some, 8 if i else 2, 61 - 2 * i)
        gathered = [gather(value) for value in mine]
        scales = pack(gate_scale[None], up_scale[None])
        ranks = list(range(chips))
        early = load(slots, mates, chips, ranks[:-1], fa, fb)
        first = min(fa + 1, fs)
        local = gate_weight.shape[0]
        close, far, totals = [], [], []
        for pieces in gathered:
            placed = [((dy * fa + dx) * local + row, v) for row, dx, dy, v in pieces]
            placed.sort(key=lambda item: item[0])
            close.append([v for row, v in placed if row < first * local])
            far.append([item for item in placed if item[0] >= first * local])
        for some in close:
            totals += near(early, [some])
        late = load(slots, mates, chips, ranks[-1:], fa, fb)
        ends = near(late, close)
        hidden = None
        for j, (at, c) in enumerate(parts):
            sums = (totals[j], ends[j])
            if j == len(parts) - 1 and j > 1 and fb == 2:
                ready = [item for item in far[j] if item[0] % local]
                far[j] = [item for item in far[j] if item[0] % local == 0]
                sums = extend((early, late), sums, ready)
            hidden = final((early, late), sums, far[j], scales, hidden, at, c, chips, width)
        return (hidden, stream)

    return jax.shard_map(
        on_device,
        mesh=mesh,
        in_specs=(
            P(("fs", "tp"), None),
            P(("fs", "tp"), None),
            P(),
            P(),
            P("fs", "tp"),
            P("fs", "tp"),
            P("tp"),
            P("tp"),
        ),
        out_specs=(P("fs", "tp"), P(("fs", "tp"), None)),
        check_vma=False,
    )
```
